32 devices in a mesh: fs: 4 (over z), rep: 4 (over y, x), tp: 2 (over core).
Axes of the slice: x: 2, y: 2, z: 4, core: 2. Of those that a mesh axis runs over, the one named last changes fastest.
Arguments:
- normed_in: bfloat16 [24576, 2048], P(('fs', 'rep')), may hold values from -6 to 6
- cotan_rec: bfloat16 [24576, 2048], P(('fs', 'rep'), 'tp'), may hold values from -0.0390625 to 0.0390625
- cotan_gate: bfloat16 [24576, 2048], P(('fs', 'rep'), 'tp'), may hold values from -0.0390625 to 0.0390625
- factor_rec: bfloat16 [2048, 512], P('fs'), may hold values from -0.125 to 0.125
- factor_gate: bfloat16 [2048, 512], P('fs'), may hold values from -0.125 to 0.125
- first_rec: float32 [512, 2048], P('fs', 'tp'), may hold values from -6 to 6
- first_gate: float32 [512, 2048], P('fs', 'tp'), may hold values from -6 to 6
- second_rec: float32 [512, 2048], P('fs', 'tp'), may hold values from 0.25 to 4
- second_gate: float32 [512, 2048], P('fs', 'tp'), may hold values from 0.25 to 4
- master_rec: float32 [2048, 2048], P('fs', 'tp'), may hold values from -0.125 to 0.125
- master_gate: float32 [2048, 2048], P('fs', 'tp'), may hold values from -0.125 to 0.125
Outputs:
- update_rec: float32 [2048, 2048], P('fs', 'tp')
- update_gate: float32 [2048, 2048], P('fs', 'tp')
- new_first_rec: float32 [512, 2048], P('fs', 'tp')
- new_first_gate: float32 [512, 2048], P('fs', 'tp')
- new_second_rec: float32 [512, 2048], P('fs', 'tp')
- new_second_gate: float32 [512, 2048], P('fs', 'tp')
- copy_rec: bfloat16 [2048, 2048], P(None, 'tp')
- copy_gate: bfloat16 [2048, 2048], P(None, 'tp')
The draws below stay inside these ranges and needn't reach their ends.
All inputs are finite; a program needn't handle non-finite values.
Results may differ from the reference program's by a relative error of at most 0.007.
Values may be sent and summed in bfloat16 or wider, within the bound.
A program may use at most 128 MiB of HBM per device.

```python
import math
import jax
import jax.numpy as jnp
from jax import lax

D = 2048
DR = 2048
RANK = 512
TOKENS = 24576


def shard_levels(stream_key, shape, pieces, smallest, largest):
    loudness, own = 1.0, jax.random.fold_in(stream_key, 6)
    for axis_at, shards_of in pieces:
        heights = jnp.exp(jax.random.uniform(jax.random.fold_in(own, axis_at), (shards_of,), jnp.float32, smallest / len(pieces), largest / len(pieces)))
        loudness = loudness * jnp.repeat(heights, shape[axis_at] // shards_of).reshape([-1 if axis == axis_at else 1 for axis in range(len(shape))])
    return loudness


def centred(key, shape, scale, limit, cuts=(), dtype=jnp.bfloat16):
    factor_of = shard_levels(key, shape, cuts, -0.22, 0.18) if cuts else 1.0
    drawn = jax.random.normal(key, shape, jnp.float32) * scale * factor_of
    return jnp.minimum(jnp.maximum(drawn, -limit), limit).astype(dtype)


def setup_inputs(seed: int = 0) -> dict:
    key_of = jax.random.split(jax.random.key(seed), 12)
    return {
        "normed_in": centred(key_of[0], (TOKENS, D), 1.0, 6.0, ((0, 16),)),
        "cotan_rec": centred(key_of[1], (TOKENS, DR), (TOKENS ** -0.5), 0.0390625, ((0, 16), (1, 2))),
        "cotan_gate": centred(key_of[2], (TOKENS, DR), (TOKENS ** -0.5), 0.0390625, ((0, 16), (1, 2))),
        "factor_rec": centred(key_of[3], (D, RANK), D ** -0.5, 0.125, ((0, 4),)),
        "factor_gate": centred(key_of[4], (D, RANK), D ** -0.5, 0.125, ((0, 4),)),
        "first_rec": centred(key_of[5], (RANK, DR), 1.0, 6.0, ((0, 4), (1, 2)), jnp.float32),
        "first_gate": centred(key_of[6], (RANK, DR), 1.0, 6.0, ((0, 4), (1, 2)), jnp.float32),
        "second_rec": jnp.clip(jnp.exp(math.log(4.0) - 2.7725887 * jax.random.uniform(key_of[7], (RANK, DR), jnp.float32) ** shard_levels(key_of[7], (RANK, DR), ((0, 4), (1, 2)), -0.2, 0.2)), 0.25, 4.0),
        "second_gate": jnp.clip(jnp.exp(math.log(4.0) - 2.7725887 * jax.random.uniform(key_of[8], (RANK, DR), jnp.float32) ** shard_levels(key_of[8], (RANK, DR), ((0, 4), (1, 2)), -0.2, 0.2)), 0.25, 4.0),
        "master_rec": centred(key_of[9], (D, DR), D ** -0.5, 0.125, ((0, 4), (1, 2)), jnp.float32),
        "master_gate": centred(key_of[10], (D, DR), D ** -0.5, 0.125, ((0, 4), (1, 2)), jnp.float32),
    }


beta_first = 0.8
beta_second = 0.9
scale_floor = 0.25
step_rate = 0.01

def project_update(normed_in, cotan, factor, first, second, master):
    grad = lax.dot_general(normed_in, cotan, (((0,), (0,)), ((), ())), preferred_element_type=jnp.float32)
    factor_wide = factor.astype(jnp.float32)
    low = jnp.dot(factor_wide.T, grad, precision=lax.Precision.HIGHEST)
    new_first = beta_first * first + (1.0 - beta_first) * low
    new_second = beta_second * second + (1.0 - beta_second) * low * low
    direction = new_first / jnp.sqrt(new_second)
    scale = 1.0 / jnp.sqrt(jnp.mean(direction * direction) + scale_floor)
    update = jnp.dot(factor_wide, direction, precision=lax.Precision.HIGHEST) * scale
    copy = (master - step_rate * update).astype(jnp.bfloat16)
    return (update, new_first, new_second, copy)

def reference(normed_in, cotan_rec, cotan_gate, factor_rec, factor_gate, first_rec, first_gate, second_rec, second_gate, master_rec, master_gate):
    upd_rec, first_r, second_r, copy_rec = project_update(normed_in, cotan_rec, factor_rec, first_rec, second_rec, master_rec)
    upd_gate, first_g, second_g, copy_gate = project_update(normed_in, cotan_gate, factor_gate, first_gate, second_gate, master_gate)
    return (upd_rec, upd_gate, first_r, first_g, second_r, second_g, copy_rec, copy_gate)
```

```python
import functools

import jax
import jax.numpy as jnp
from jax import lax
from jax.experimental import pallas as pl
from jax.experimental.pallas import tpu as pltpu
from jax.sharding import PartitionSpec as P

beta_first = 0.8
beta_second = 0.9
scale_floor = 0.25
step_rate = 0.01

MESH = pl.DeviceIdType.MESH
F32 = jnp.float32
BF16 = jnp.bfloat16
TOKEN_TILES = 4


def kernel(
    nf,
    nr,
    x_hbm,
    c0_hbm,
    c1_hbm,
    fac0_hbm,
    fac1_hbm,
    first0,
    first1,
    second0,
    second1,
    fac_out,
    dir_out,
    low_out,
    sum_out,
    x,
    c,
    fac,
    proj,
    part,
    own,
    recv_rep,
    mid,
    recv_fs,
    fst,
    snd,
    low,
    dirs,
    sums,
    sums_in,
    local_sem,
    out_sem,
    fz_s,
    fz_r,
    fr_s,
    fr_r,
    fx_s,
    fx_r,
    pj_s,
    pj_r,
    rr_s,
    rr_r,
    rf_s,
    rf_r,
    dz_s,
    dz_r,
    dr_s,
    dr_r,
    lw_s,
    lw_r,
    sm_s,
    sm_r,
):
    f, r, t = lax.axis_index("fs"), lax.axis_index("rep"), lax.axis_index("tp")
    tokens = x.shape[0]
    rank, cols = dirs.shape[1], dirs.shape[2]
    rows = fac0_hbm.shape[0]
    quarter = rows // nr
    low_rows = rank // nf
    width = cols // nr
    tile = tokens // TOKEN_TILES

    def fpeer(k):
        return lax.rem(f + k, nf)

    def rpeer(k):
        return lax.rem(r + k, nr)

    mine = fac.at[t, pl.ds(pl.multiple_of(f * rows, rows), rows), :]

    @pl.when(t == 0)
    def _():
        pltpu.make_async_copy(fac0_hbm, mine, local_sem.at[0]).start()

    @pl.when(t != 0)
    def _():
        pltpu.make_async_copy(fac1_hbm, mine, local_sem.at[0]).start()

    load_x = pltpu.make_async_copy(x_hbm, x, local_sem.at[1])
    load_x.start()
    loads = [
        pltpu.make_async_copy(c0_hbm, c.at[0], local_sem.at[2]),
        pltpu.make_async_copy(c1_hbm, c.at[1], local_sem.at[3]),
    ]
    lane = pl.ds(pl.multiple_of(r * width, width), width)
    for i, (src, dst) in enumerate(
        ((first0, fst.at[0]), (first1, fst.at[1]), (second0, snd.at[0]), (second1, snd.at[1]))
    ):
        loads.append(pltpu.make_async_copy(src.at[:, lane], dst, local_sem.at[4 + i]))
    for load in loads:
        load.start()

    barrier = pltpu.get_barrier_semaphore()
    for k in range(1, nf):
        pl.semaphore_signal(barrier, inc=1, device_id=(fpeer(k), r, t), device_id_type=MESH)
    for k in range(1, nr):
        pl.semaphore_signal(barrier, inc=1, device_id=(f, rpeer(k), t), device_id_type=MESH)
    pl.semaphore_signal(barrier, inc=1, device_id=(f, r, 1 - t), device_id_type=MESH)
    pl.semaphore_wait(barrier, nf + nr - 1)

    started = []

    def send(src, dst, s_sem, r_sem, device):
        copy = pltpu.make_async_remote_copy(
            src_ref=src, dst_ref=dst, send_sem=s_sem, recv_sem=r_sem,
            device_id=device, device_id_type=MESH,
        )
        copy.start()
        started.append(copy)

    def arrived(ref, s_sem, r_sem, device):
        pltpu.make_async_remote_copy(
            src_ref=ref, dst_ref=ref, send_sem=s_sem, recv_sem=r_sem,
            device_id=device, device_id_type=MESH,
        ).wait_recv()

    sibling = (f, r, 1 - t)

    def fpiece(ff, rr):
        start = pl.multiple_of(ff * rows + rr * quarter, quarter)
        return fac.at[t, pl.ds(start, quarter), :]

    pltpu.make_async_copy(fac0_hbm, mine, local_sem.at[0]).wait()
    for k in range(1, nf):
        send(fpiece(f, r), fpiece(f, r), fz_s.at[k - 1], fz_r.at[k - 1], (fpeer(k), r, t))
    for k in range(1, nf):
        src = fpeer(nf - k)
        arrived(fpiece(src, r), fz_s.at[k - 1], fz_r.at[k - 1], (src, r, t))
        for j in range(1, nr):
            send(fpiece(src, r), fpiece(src, r), fr_s.at[k - 1, j - 1], fr_r.at[k - 1, j - 1], (f, rpeer(j), t))
    for k in range(1, nf):
        src = fpeer(nf - k)
        for j in range(1, nr):
            rsrc = rpeer(nr - j)
            arrived(fpiece(src, rsrc), fr_s.at[k - 1, j - 1], fr_r.at[k - 1, j - 1], (f, rsrc, t))

    load_x.wait()
    for i in range(TOKEN_TILES):
        span = pl.ds(i * tile, tile)
        proj[t, span, :] = jnp.dot(
            x[span, :], fac[t], preferred_element_type=F32
        ).astype(BF16)
        send(proj.at[t, span, :], proj.at[t, span, :], pj_s.at[i], pj_r.at[i], sibling)
    send(fac.at[t], fac.at[t], fx_s, fx_r, sibling)
    for load in loads:
        load.wait()

    def product(p, rr):
        at = pl.ds(pl.multiple_of(rr * width, width), width)
        return lax.dot_general(
            proj[p], c[p, :, at], (((0,), (0,)), ((), ())), preferred_element_type=F32
        )

    order = (t, 1 - t)
    for s, p in enumerate(order):
        if s == 1:
            for i in range(TOKEN_TILES):
                span = pl.ds(i * tile, tile)
                arrived(proj.at[1 - t, span, :], pj_s.at[i], pj_r.at[i], sibling)
        for j in range(1, nr):
            part[s, j - 1] = product(p, rpeer(j)).astype(BF16)
            send(part.at[s, j - 1], recv_rep.at[s, j - 1], rr_s.at[s, j - 1], rr_r.at[s, j - 1], (f, rpeer(j), t))
        own[s] = product(p, r)

    def rank_rows(ff):
        return pl.ds(pl.multiple_of(ff * low_rows, low_rows), low_rows)

    for s in range(2):
        for j in range(1, nr):
            arrived(recv_rep.at[s, j - 1], rr_s.at[s, j - 1], rr_r.at[s, j - 1], (f, rpeer(nr - j), t))
        total = own[s]
        for j in range(1, nr):
            total = total + recv_rep[s, j - 1].astype(F32)
        own[s] = total
        mid[s] = total.astype(BF16)
        for k in range(1, nf):
            send(mid.at[s, rank_rows(fpeer(k)), :], recv_fs.at[s, k - 1], rf_s.at[s, k - 1], rf_r.at[s, k - 1], (fpeer(k), r, t))

    def dpiece(p, ff, rr):
        at = pl.ds(pl.multiple_of(rr * width, width), width)
        return dirs.at[p, rank_rows(ff), at]

    for s, p in enumerate(order):
        for k in range(1, nf):
            arrived(recv_fs.at[s, k - 1], rf_s.at[s, k - 1], rf_r.at[s, k - 1], (fpeer(nf - k), r, t))
        total = own[s, rank_rows(f), :]
        for k in range(1, nf):
            total = total + recv_fs[s, k - 1].astype(F32)
        rounded = total.astype(BF16)
        low[p, :, lane] = rounded
        wide = rounded.astype(F32)
        new_first = beta_first * fst[p] + (1.0 - beta_first) * wide
        new_second = beta_second * snd[p] + (1.0 - beta_second) * wide * wide
        dirs[p, rank_rows(f), lane] = (new_first / jnp.sqrt(new_second)).astype(BF16)
        for k in range(1, nf):
            send(dpiece(p, f, r), dpiece(p, f, r), dz_s.at[s, k - 1], dz_r.at[s, k - 1], (fpeer(k), r, t))
        for j in range(1, nr):
            send(dpiece(p, f, r), dpiece(p, f, r), dr_s.at[s, 0, j - 1], dr_r.at[s, 0, j - 1], (f, rpeer(j), t))
    for s, p in enumerate(order):
        for k in range(1, nf):
            src = fpeer(nf - k)
            arrived(dpiece(p, src, r), dz_s.at[s, k - 1], dz_r.at[s, k - 1], (src, r, t))
            for j in range(1, nr):
                send(dpiece(p, src, r), dpiece(p, src, r), dr_s.at[s, k, j - 1], dr_r.at[s, k, j - 1], (f, rpeer(j), t))
    for j in range(1, nr):
        send(low.at[:, :, lane], low.at[:, :, lane], lw_s.at[j - 1], lw_r.at[j - 1], (f, rpeer(j), t))

    outs = []

    def put(src, dst):
        copy = pltpu.make_async_copy(src, dst, out_sem.at[len(outs)])
        copy.start()
        outs.append(copy)

    arrived(fac.at[1 - t], fx_s, fx_r, sibling)
    put(fac, fac_out)
    for s, p in enumerate(order):
        for k in range(nf):
            src = fpeer(nf - k)
            for j in range(1, nr):
                rsrc = rpeer(nr - j)
                arrived(dpiece(p, src, rsrc), dr_s.at[s, k, j - 1], dr_r.at[s, k, j - 1], (f, rsrc, t))
    put(dirs, dir_out)

    for p in range(2):
        square = dirs[p].astype(F32)
        square = square * square
        sums[p] = jnp.sum(square.reshape(rank // 8, 8, cols), axis=0)
    send(sums, sums_in, sm_s, sm_r, sibling)
    for j in range(1, nr):
        rsrc = rpeer(nr - j)
        at = pl.ds(pl.multiple_of(rsrc * width, width), width)
        arrived(low.at[:, :, at], lw_s.at[j - 1], lw_r.at[j - 1], (f, rsrc, t))
    put(low, low_out)
    arrived(sums_in, sm_s, sm_r, sibling)
    for p in range(2):
        sum_out[p] = sums[p] + sums_in[p]
    for copy in outs:
        copy.wait()
    for copy in started:
        copy.wait_send()


def gather_directions(nf, nr, normed_in, cotans, factors, firsts, seconds):
    tokens, model = normed_in.shape
    cols = cotans[0].shape[1]
    rows, rank = factors[0].shape
    low_rows, width = rank // nf, cols // nr
    dma = pltpu.SemaphoreType.DMA
    anyspec = pl.BlockSpec(memory_space=pl.ANY)
    pair = lambda *shape: [dma(shape), dma(shape)]
    return pl.pallas_call(
        functools.partial(kernel, nf, nr),
        out_shape=(
            jax.ShapeDtypeStruct((2, model, rank), BF16),
            jax.ShapeDtypeStruct((2, rank, cols), BF16),
            jax.ShapeDtypeStruct((2, low_rows, cols), BF16),
            jax.ShapeDtypeStruct((2, 8, cols), F32),
        ),
        in_specs=[anyspec] * 9,
        out_specs=(anyspec, anyspec, anyspec, pl.BlockSpec(memory_space=pltpu.VMEM)),
        scratch_shapes=[
            pltpu.VMEM((tokens, model), BF16),
            pltpu.VMEM((2, tokens, cols), BF16),
            pltpu.VMEM((2, model, rank), BF16),
            pltpu.VMEM((2, tokens, rank), BF16),
            pltpu.VMEM((2, nr - 1, rank, width), BF16),
            pltpu.VMEM((2, rank, width), F32),
            pltpu.VMEM((2, nr - 1, rank, width), BF16),
            pltpu.VMEM((2, rank, width), BF16),
            pltpu.VMEM((2, nf - 1, low_rows, width), BF16),
            pltpu.VMEM((2, low_rows, width), F32),
            pltpu.VMEM((2, low_rows, width), F32),
            pltpu.VMEM((2, low_rows, cols), BF16),
            pltpu.VMEM((2, rank, cols), BF16),
            pltpu.VMEM((2, 8, cols), F32),
            pltpu.VMEM((2, 8, cols), F32),
            dma((8,)),
            dma((3,)),
            *pair(nf - 1),
            *pair(nf - 1, nr - 1),
            dma,
            dma,
            *pair(TOKEN_TILES),
            *pair(2, nr - 1),
            *pair(2, nf - 1),
            *pair(2, nf - 1),
            *pair(2, nf, nr - 1),
            *pair(nr - 1),
            dma,
            dma,
        ],
        cost_estimate=pl.CostEstimate(
            flops=10 * tokens * model * rank, bytes_accessed=400 * 2**20, transcendentals=0
        ),
        compiler_params=pltpu.CompilerParams(
            collective_id=0, has_side_effects=True, vmem_limit_bytes=48 * 2**20
        ),
    )(normed_in, *cotans, *factors, *firsts, *seconds)


def body(
    nf,
    nr,
    nt,
    normed_in,
    cotan_rec,
    cotan_gate,
    factor_rec,
    factor_gate,
    first_rec,
    first_gate,
    second_rec,
    second_gate,
    master_rec,
    master_gate,
):
    r = lax.axis_index("rep")
    factors = (factor_rec, factor_gate)
    firsts = (first_rec, first_gate)
    seconds = (second_rec, second_gate)
    piece = master_rec.shape[0] // nr
    wholes = [
        lax.all_gather(
            lax.dynamic_slice_in_dim(m, r * piece, piece, 0).astype(BF16),
            ("fs", "rep"), axis=0, tiled=True,
        )
        for m in (master_rec, master_gate)
    ]
    fac, dirs, low, sums = gather_directions(
        nf, nr, normed_in, (cotan_rec, cotan_gate), factors, firsts, seconds
    )
    entries = float(dirs.shape[1] * dirs.shape[2] * nt)
    updates, new_firsts, new_seconds, copies = [], [], [], []
    for p in range(2):
        scale = 1.0 / jnp.sqrt(jnp.sum(sums[p]) / entries + scale_floor)
        updates.append(jnp.dot(factors[p], dirs[p], preferred_element_type=F32) * scale)
        wide = low[p].astype(F32)
        new_firsts.append(beta_first * firsts[p] + (1.0 - beta_first) * wide)
        new_seconds.append(beta_second * seconds[p] + (1.0 - beta_second) * wide * wide)
        upd = jnp.dot(fac[p], dirs[p], preferred_element_type=F32) * scale
        copies.append((wholes[p].astype(F32) - step_rate * upd).astype(BF16))
    return (*updates, *new_firsts, *new_seconds, *copies)


def solution(mesh):
    nf, nr, nt = mesh.shape["fs"], mesh.shape["rep"], mesh.shape["tp"]
    return jax.shard_map(
        functools.partial(body, nf, nr, nt),
        mesh=mesh,
        in_specs=(
            P(("fs", "rep"), None),
            P(("fs", "rep"), "tp"),
            P(("fs", "rep"), "tp"),
            P("fs", None),
            P("fs", None),
            P("fs", "tp"),
            P("fs", "tp"),
            P("fs", "tp"),
            P("fs", "tp"),
            P("fs", "tp"),
            P("fs", "tp"),
        ),
        out_specs=(
            P("fs", "tp"),
            P("fs", "tp"),
            P("fs", "tp"),
            P("fs", "tp"),
            P("fs", "tp"),
            P("fs", "tp"),
            P(None, "tp"),
            P(None, "tp"),
        ),
        check_vma=False,
    )
```

```python
import functools

import jax
import jax.numpy as jnp
from jax import lax
from jax.experimental import pallas as pl
from jax.experimental.pallas import tpu as pltpu
from jax.sharding import PartitionSpec as P

beta_first = 0.8
beta_second = 0.9
scale_floor = 0.25
step_rate = 0.01

MESH = pl.DeviceIdType.MESH
F32 = jnp.float32
BF16 = jnp.bfloat16
TOKEN_TILES = 4


def kernel(
    nf,
    nr,
    x_hbm,
    c0_hbm,
    c1_hbm,
    fac0_hbm,
    fac1_hbm,
    first0,
    first1,
    second0,
    second1,
    mast_hbm,
    fac_out,
    dir_out,
    low_out,
    mast_out,
    sum_out,
    x,
    c,
    fac,
    proj,
    part,
    own,
    recv_rep,
    mid,
    recv_fs,
    fst,
    snd,
    low,
    dirs,
    sums,
    sums_in,
    mast,
    local_sem,
    out_sem,
    fz_s,
    fz_r,
    fr_s,
    fr_r,
    fx_s,
    fx_r,
    pj_s,
    pj_r,
    rr_s,
    rr_r,
    rf_s,
    rf_r,
    dz_s,
    dz_r,
    dr_s,
    dr_r,
    lw_s,
    lw_r,
    sm_s,
    sm_r,
    mz_s,
    mz_r,
    mr_s,
    mr_r,
):
    f, r, t = lax.axis_index("fs"), lax.axis_index("rep"), lax.axis_index("tp")
    tokens = x.shape[0]
    rank, cols = dirs.shape[1], dirs.shape[2]
    rows = fac0_hbm.shape[0]
    quarter = rows // nr
    low_rows = rank // nf
    width = cols // nr
    tile = tokens // TOKEN_TILES

    def fpeer(k):
        return lax.rem(f + k, nf)

    def rpeer(k):
        return lax.rem(r + k, nr)

    mine = fac.at[t, pl.ds(pl.multiple_of(f * rows, rows), rows), :]

    @pl.when(t == 0)
    def _():
        pltpu.make_async_copy(fac0_hbm, mine, local_sem.at[0]).start()

    @pl.when(t != 0)
    def _():
        pltpu.make_async_copy(fac1_hbm, mine, local_sem.at[0]).start()

    load_m = pltpu.make_async_copy(
        mast_hbm, mast.at[pl.ds(pl.multiple_of(f * rows, rows), rows), :], local_sem.at[8]
    )
    load_m.start()
    load_x = pltpu.make_async_copy(x_hbm, x, local_sem.at[1])
    load_x.start()
    loads = [
        pltpu.make_async_copy(c0_hbm, c.at[0], local_sem.at[2]),
        pltpu.make_async_copy(c1_hbm, c.at[1], local_sem.at[3]),
    ]
    lane = pl.ds(pl.multiple_of(r * width, width), width)
    for i, (src, dst) in enumerate(
        ((first0, fst.at[0]), (first1, fst.at[1]), (second0, snd.at[0]), (second1, snd.at[1]))
    ):
        loads.append(pltpu.make_async_copy(src.at[:, lane], dst, local_sem.at[4 + i]))
    for load in loads:
        load.start()

    barrier = pltpu.get_barrier_semaphore()
    for k in range(1, nf):
        pl.semaphore_signal(barrier, inc=1, device_id=(fpeer(k), r, t), device_id_type=MESH)
    for k in range(1, nr):
        pl.semaphore_signal(barrier, inc=1, device_id=(f, rpeer(k), t), device_id_type=MESH)
    pl.semaphore_signal(barrier, inc=1, device_id=(f, r, 1 - t), device_id_type=MESH)
    pl.semaphore_wait(barrier, nf + nr - 1)

    started = []

    def send(src, dst, s_sem, r_sem, device):
        copy = pltpu.make_async_remote_copy(
            src_ref=src, dst_ref=dst, send_sem=s_sem, recv_sem=r_sem,
            device_id=device, device_id_type=MESH,
        )
        copy.start()
        started.append(copy)

    def arrived(ref, s_sem, r_sem, device):
        pltpu.make_async_remote_copy(
            src_ref=ref, dst_ref=ref, send_sem=s_sem, recv_sem=r_sem,
            device_id=device, device_id_type=MESH,
        ).wait_recv()

    sibling = (f, r, 1 - t)

    def fpiece(ff, rr):
        start = pl.multiple_of(ff * rows + rr * quarter, quarter)
        return fac.at[t, pl.ds(start, quarter), :]

    pltpu.make_async_copy(fac0_hbm, mine, local_sem.at[0]).wait()
    for k in range(1, nf):
        send(fpiece(f, r), fpiece(f, r), fz_s.at[k - 1], fz_r.at[k - 1], (fpeer(k), r, t))

    def mpiece(ff, rr):
        start = pl.multiple_of(ff * rows + rr * quarter, quarter)
        return mast.at[pl.ds(start, quarter), :]

    def pass_master(k):
        src = fpeer(nf - k)
        arrived(mpiece(src, r), mz_s.at[k - 1], mz_r.at[k - 1], (src, r, t))
        for j in range(1, nr):
            send(mpiece(src, r), mpiece(src, r), mr_s.at[k - 1, j - 1], mr_r.at[k - 1, j - 1], (f, rpeer(j), t))

    third = (nf - 1) // 3
    load_m.wait()
    for k in range(1, nf):
        send(mpiece(f, r), mpiece(f, r), mz_s.at[k - 1], mz_r.at[k - 1], (fpeer(k), r, t))
    for k in range(1, nf):
        src = fpeer(nf - k)
        arrived(fpiece(src, r), fz_s.at[k - 1], fz_r.at[k - 1], (src, r, t))
        for j in range(1, nr):
            send(fpiece(src, r), fpiece(src, r), fr_s.at[k - 1, j - 1], fr_r.at[k - 1, j - 1], (f, rpeer(j), t))
    for k in range(1, nf):
        src = fpeer(nf - k)
        for j in range(1, nr):
            rsrc = rpeer(nr - j)
            arrived(fpiece(src, rsrc), fr_s.at[k - 1, j - 1], fr_r.at[k - 1, j - 1], (f, rsrc, t))

    for k in range(1, 1 + third):
        pass_master(k)

    load_x.wait()
    for i in range(TOKEN_TILES):
        span = pl.ds(i * tile, tile)
        proj[t, span, :] = jnp.dot(
            x[span, :], fac[t], preferred_element_type=F32
        ).astype(BF16)
        send(proj.at[t, span, :], proj.at[t, span, :], pj_s.at[i], pj_r.at[i], sibling)
    send(fac.at[t], fac.at[t], fx_s, fx_r, sibling)
    for load in loads:
        load.wait()

    def product(p, rr):
        at = pl.ds(pl.multiple_of(rr * width, width), width)
        return lax.dot_general(
            proj[p], c[p, :, at], (((0,), (0,)), ((), ())), preferred_element_type=F32
        )

    order = (t, 1 - t)
    for s, p in enumerate(order):
        if s == 1:
            for i in range(TOKEN_TILES):
                span = pl.ds(i * tile, tile)
                arrived(proj.at[1 - t, span, :], pj_s.at[i], pj_r.at[i], sibling)
        for j in range(1, nr):
            part[s, j - 1] = product(p, rpeer(j)).astype(BF16)
            send(part.at[s, j - 1], recv_rep.at[s, j - 1], rr_s.at[s, j - 1], rr_r.at[s, j - 1], (f, rpeer(j), t))
        own[s] = product(p, r)

    for k in range(1 + third, 1 + 2 * third):
        pass_master(k)

    def rank_rows(ff):
        return pl.ds(pl.multiple_of(ff * low_rows, low_rows), low_rows)

    for s in range(2):
        for j in range(1, nr):
            arrived(recv_rep.at[s, j - 1], rr_s.at[s, j - 1], rr_r.at[s, j - 1], (f, rpeer(nr - j), t))
        total = own[s]
        for j in range(1, nr):
            total = total + recv_rep[s, j - 1].astype(F32)
        own[s] = total
        mid[s] = total.astype(BF16)
        for k in range(1, nf):
            send(mid.at[s, rank_rows(fpeer(k)), :], recv_fs.at[s, k - 1], rf_s.at[s, k - 1], rf_r.at[s, k - 1], (fpeer(k), r, t))

    def dpiece(p, ff, rr):
        at = pl.ds(pl.multiple_of(rr * width, width), width)
        return dirs.at[p, rank_rows(ff), at]

    for s, p in enumerate(order):
        for k in range(1, nf):
            arrived(recv_fs.at[s, k - 1], rf_s.at[s, k - 1], rf_r.at[s, k - 1], (fpeer(nf - k), r, t))
        total = own[s, rank_rows(f), :]
        for k in range(1, nf):
            total = total + recv_fs[s, k - 1].astype(F32)
        rounded = total.astype(BF16)
        low[p, :, lane] = rounded
        wide = rounded.astype(F32)
        new_first = beta_first * fst[p] + (1.0 - beta_first) * wide
        new_second = beta_second * snd[p] + (1.0 - beta_second) * wide * wide
        dirs[p, rank_rows(f), lane] = (new_first / jnp.sqrt(new_second)).astype(BF16)
        for k in range(1, nf):
            send(dpiece(p, f, r), dpiece(p, f, r), dz_s.at[s, k - 1], dz_r.at[s, k - 1], (fpeer(k), r, t))
        for j in range(1, nr):
            send(dpiece(p, f, r), dpiece(p, f, r), dr_s.at[s, 0, j - 1], dr_r.at[s, 0, j - 1], (f, rpeer(j), t))
    for k in range(1 + 2 * third, nf):
        pass_master(k)
    for s, p in enumerate(order):
        for k in range(1, nf):
            src = fpeer(nf - k)
            arrived(dpiece(p, src, r), dz_s.at[s, k - 1], dz_r.at[s, k - 1], (src, r, t))
            for j in range(1, nr):
                send(dpiece(p, src, r), dpiece(p, src, r), dr_s.at[s, k, j - 1], dr_r.at[s, k, j - 1], (f, rpeer(j), t))
    for j in range(1, nr):
        send(low.at[:, :, lane], low.at[:, :, lane], lw_s.at[j - 1], lw_r.at[j - 1], (f, rpeer(j), t))

    outs = []

    def put(src, dst):
        copy = pltpu.make_async_copy(src, dst, out_sem.at[len(outs)])
        copy.start()
        outs.append(copy)

    arrived(fac.at[1 - t], fx_s, fx_r, sibling)
    put(fac, fac_out)
    for s, p in enumerate(order):
        for k in range(nf):
            src = fpeer(nf - k)
            for j in range(1, nr):
                rsrc = rpeer(nr - j)
                arrived(dpiece(p, src, rsrc), dr_s.at[s, k, j - 1], dr_r.at[s, k, j - 1], (f, rsrc, t))
    put(dirs, dir_out)

    for p in range(2):
        square = dirs[p].astype(F32)
        square = square * square
        sums[p] = jnp.sum(square.reshape(rank // 8, 8, cols), axis=0)
    send(sums, sums_in, sm_s, sm_r, sibling)
    for j in range(1, nr):
        rsrc = rpeer(nr - j)
        at = pl.ds(pl.multiple_of(rsrc * width, width), width)
        arrived(low.at[:, :, at], lw_s.at[j - 1], lw_r.at[j - 1], (f, rsrc, t))
    put(low, low_out)
    for k in range(1, nf):
        src = fpeer(nf - k)
        for j in range(1, nr):
            rsrc = rpeer(nr - j)
            arrived(mpiece(src, rsrc), mr_s.at[k - 1, j - 1], mr_r.at[k - 1, j - 1], (f, rsrc, t))
    put(mast, mast_out)
    arrived(sums_in, sm_s, sm_r, sibling)
    for p in range(2):
        sum_out[p] = sums[p] + sums_in[p]
    for copy in outs:
        copy.wait()
    for copy in started:
        copy.wait_send()


def gather_directions(nf, nr, normed_in, cotans, factors, firsts, seconds, master):
    tokens, model = normed_in.shape
    cols = cotans[0].shape[1]
    rows, rank = factors[0].shape
    low_rows, width = rank // nf, cols // nr
    dma = pltpu.SemaphoreType.DMA
    anyspec = pl.BlockSpec(memory_space=pl.ANY)
    pair = lambda *shape: [dma(shape), dma(shape)]
    return pl.pallas_call(
        functools.partial(kernel, nf, nr),
        out_shape=(
            jax.ShapeDtypeStruct((2, model, rank), BF16),
            jax.ShapeDtypeStruct((2, rank, cols), BF16),
            jax.ShapeDtypeStruct((2, low_rows, cols), BF16),
            jax.ShapeDtypeStruct((model, master.shape[1]), BF16),
            jax.ShapeDtypeStruct((2, 8, cols), F32),
        ),
        in_specs=[anyspec] * 10,
        out_specs=(anyspec, anyspec, anyspec, anyspec, pl.BlockSpec(memory_space=pltpu.VMEM)),
        scratch_shapes=[
            pltpu.VMEM((tokens, model), BF16),
            pltpu.VMEM((2, tokens, cols), BF16),
            pltpu.VMEM((2, model, rank), BF16),
            pltpu.VMEM((2, tokens, rank), BF16),
            pltpu.VMEM((2, nr - 1, rank, width), BF16),
            pltpu.VMEM((2, rank, width), F32),
            pltpu.VMEM((2, nr - 1, rank, width), BF16),
            pltpu.VMEM((2, rank, width), BF16),
            pltpu.VMEM((2, nf - 1, low_rows, width), BF16),
            pltpu.VMEM((2, low_rows, width), F32),
            pltpu.VMEM((2, low_rows, width), F32),
            pltpu.VMEM((2, low_rows, cols), BF16),
            pltpu.VMEM((2, rank, cols), BF16),
            pltpu.VMEM((2, 8, cols), F32),
            pltpu.VMEM((2, 8, cols), F32),
            pltpu.VMEM((model, master.shape[1]), BF16),
            dma((9,)),
            dma((4,)),
            *pair(nf - 1),
            *pair(nf - 1, nr - 1),
            dma,
            dma,
            *pair(TOKEN_TILES),
            *pair(2, nr - 1),
            *pair(2, nf - 1),
            *pair(2, nf - 1),
            *pair(2, nf, nr - 1),
            *pair(nr - 1),
            dma,
            dma,
            *pair(nf - 1),
            *pair(nf - 1, nr - 1),
        ],
        cost_estimate=pl.CostEstimate(
            flops=10 * tokens * model * rank, bytes_accessed=400 * 2**20, transcendentals=0
        ),
        compiler_params=pltpu.CompilerParams(
            collective_id=0, has_side_effects=True, vmem_limit_bytes=60 * 2**20
        ),
    )(normed_in, *cotans, *factors, *firsts, *seconds, master)


def body(
    nf,
    nr,
    nt,
    normed_in,
    cotan_rec,
    cotan_gate,
    factor_rec,
    factor_gate,
    first_rec,
    first_gate,
    second_rec,
    second_gate,
    master_rec,
    master_gate,
):
    r = lax.axis_index("rep")
    factors = (factor_rec, factor_gate)
    firsts = (first_rec, first_gate)
    seconds = (second_rec, second_gate)
    piece = master_rec.shape[0] // nr
    half = 3 * master_gate.shape[1] // 4

    def gathered(m):
        own = lax.dynamic_slice_in_dim(m, r * piece, piece, 0).astype(BF16)
        return lax.all_gather(own, ("fs", "rep"), axis=0, tiled=True)

    whole_rec = gathered(master_rec)
    gate_right = gathered(master_gate[:, half:])
    fac, dirs, low, gate_left, sums = gather_directions(
        nf, nr, normed_in, (cotan_rec, cotan_gate), factors, firsts, seconds,
        master_gate[:, :half].astype(BF16),
    )
    wholes = (whole_rec, jnp.concatenate((gate_left, gate_right), axis=1))
    entries = float(dirs.shape[1] * dirs.shape[2] * nt)
    updates, new_firsts, new_seconds, copies = [], [], [], []
    for p in range(2):
        scale = 1.0 / jnp.sqrt(jnp.sum(sums[p]) / entries + scale_floor)
        updates.append(jnp.dot(factors[p], dirs[p], preferred_element_type=F32) * scale)
        wide = low[p].astype(F32)
        new_firsts.append(beta_first * firsts[p] + (1.0 - beta_first) * wide)
        new_seconds.append(beta_second * seconds[p] + (1.0 - beta_second) * wide * wide)
        upd = jnp.dot(fac[p], dirs[p], preferred_element_type=F32) * scale
        copies.append((wholes[p].astype(F32) - step_rate * upd).astype(BF16))
    return (*updates, *new_firsts, *new_seconds, *copies)


def solution(mesh):
    nf, nr, nt = mesh.shape["fs"], mesh.shape["rep"], mesh.shape["tp"]
    return jax.shard_map(
        functools.partial(body, nf, nr, nt),
        mesh=mesh,
        in_specs=(
            P(("fs", "rep"), None),
            P(("fs", "rep"), "tp"),
            P(("fs", "rep"), "tp"),
            P("fs", None),
            P("fs", None),
            P("fs", "tp"),
            P("fs", "tp"),
            P("fs", "tp"),
            P("fs", "tp"),
            P("fs", "tp"),
            P("fs", "tp"),
        ),
        out_specs=(
            P("fs", "tp"),
            P("fs", "tp"),
            P("fs", "tp"),
            P("fs", "tp"),
            P("fs", "tp"),
            P("fs", "tp"),
            P(None, "tp"),
            P(None, "tp"),
        ),
        check_vma=False,
    )
```
